32 devices in a mesh: fs: 4 (over z), rep: 4 (over y, x), tp: 2 (over core).
Axes of the slice: x: 2, y: 2, z: 4, core: 2. Of those that a mesh axis runs over, the one named last changes fastest.
Arguments:
- saved_input: bfloat16 [5632, 2048], P(('fs', 'rep')), may hold values from -6 to 6
- query_cot: bfloat16 [5632, 1024], P(('fs', 'rep'), 'tp'), may hold values from -0.078125 to 0.078125
- attn_out: bfloat16 [5632, 1024], P(('fs', 'rep'), 'tp'), may hold values from -6 to 6
- out_cot: bfloat16 [5632, 2048], P(('fs', 'rep')), may hold values from -0.078125 to 0.078125
- query_basis: bfloat16 [2048, 512], P('fs'), may hold values from -0.25 to 0.25
- output_basis: bfloat16 [2048, 512], P('fs'), may hold values from -0.25 to 0.25
- query_weight: float32 [2048, 1024], P('fs', 'tp'), may hold values from -6 to 6
- output_weight: float32 [1024, 2048], P('tp', 'fs'), may hold values from -6 to 6
- query_moment: float32 [512, 1024], P('rep', 'tp'), may hold values from -52 to 52
- output_moment: float32 [1024, 512], P('tp', 'rep'), may hold values from -52 to 52
Outputs:
- query_step: float32 [2048, 1024], P('fs', 'tp')
- output_step: float32 [1024, 2048], P('tp', 'fs')
- query_new: float32 [2048, 1024], P('fs', 'tp')
- output_new: float32 [1024, 2048], P('tp', 'fs')
- query_copy: bfloat16 [2048, 1024], P('fs', 'tp')
- output_copy: bfloat16 [1024, 2048], P('tp', 'fs')
- query_moment_new: float32 [512, 1024], P('rep', 'tp')
- output_moment_new: float32 [1024, 512], P('tp', 'rep')
The draws below stay inside these ranges and needn't reach their ends.
All inputs are finite; a program needn't handle non-finite values.
Results may differ from the reference program's by a relative error of at most 0.0029.
Values may be sent and summed in bfloat16 or wider, within the bound.
No kernel may reach another device: no remote copies, remote signals or barrier semaphores. Data moves between devices by JAX's collectives and lax.ppermute only.
A program may use at most 64 MiB of HBM per device.

```python
import jax
import jax.numpy as jnp
from jax import lax

D = 2048
HEADS = 16
HEAD_DIM = 64
RANK = 512
HD = 1024
TOKENS = 5632


def scaled_field(key, rows, cols):
    first = jax.random.fold_in(key, 11)
    row_pos = jnp.arange(rows, dtype=jnp.float32) / max(rows - 1, 1)
    col_pos = jnp.arange(cols, dtype=jnp.float32) / max(cols - 1, 1)
    base = jnp.clip(jax.random.normal(first, (rows, cols), jnp.float32), -3.0, 3.0)
    row_scale = 1.0 + 3.0 * row_pos
    col_scale = 1.0 + 2.0 * col_pos
    return base * row_scale[:, None] * col_scale[None, :]


def draw_query_moment(key, part):
    return scaled_field(key, RANK, HEADS * HEAD_DIM)


def draw_output_moment(key, part):
    return scaled_field(jax.random.fold_in(key, 5), HEADS * HEAD_DIM, RANK)


def levels(rng, extent, split, low, high):
    gain, own = 1.0, jax.random.fold_in(rng, 6)
    for axis_at, parts in split:
        steps = jnp.exp(jax.random.uniform(jax.random.fold_in(own, axis_at), (parts,), jnp.float32, low / len(split), high / len(split)))
        gain = gain * jnp.repeat(steps, extent[axis_at] // parts).reshape([-1 if axis == axis_at else 1 for axis in range(len(extent))])
    return gain


def scatter_about(rng, extent, scale, bound, split=(), kind=jnp.bfloat16):
    array = scale * jax.random.normal(rng, extent, jnp.float32)
    if split:
        array = array * levels(rng, extent, split, -0.22, 0.18)
    return jnp.clip(array, -bound, bound).astype(kind)


def setup_inputs(seed: int = 0) -> dict:
    splits = jax.random.split(jax.random.key(seed), 11)
    saved_input = scatter_about(splits[0], (TOKENS, D), 1.0, 6.0, ((0, 16),))
    query_cot = scatter_about(splits[1], (TOKENS, HD), (TOKENS ** -0.5), 0.078125, ((0, 16), (1, 2)))
    attn_out = scatter_about(splits[2], (TOKENS, HD), 1.0, 6.0, ((0, 16), (1, 2)))
    out_cot = scatter_about(splits[3], (TOKENS, D), (TOKENS ** -0.5), 0.078125, ((0, 16),))
    query_basis = scatter_about(splits[4], (D, RANK), RANK ** -0.5, 0.25, ((0, 4),))
    output_basis = scatter_about(splits[5], (D, RANK), RANK ** -0.5, 0.25, ((0, 4),))
    query_weight = scatter_about(splits[6], (D, HD), 1.0, 6.0, ((0, 4), (1, 2)), jnp.float32)
    output_weight = scatter_about(splits[7], (HD, D), 1.0, 6.0, ((0, 2), (1, 4)), jnp.float32)
    query_moment = draw_query_moment(jax.random.fold_in(splits[10], 71), 0)
    output_moment = draw_output_moment(jax.random.fold_in(splits[10], 71), 0)
    return dict(saved_input=saved_input, query_cot=query_cot, attn_out=attn_out, out_cot=out_cot, query_basis=query_basis, output_basis=output_basis, query_weight=query_weight, output_weight=output_weight, query_moment=query_moment, output_moment=output_moment)


BETA = 0.8
RATE = 0.2
EPS = 1e-06

def normalize(moment):
    scale = lax.rsqrt(jnp.mean(moment * moment) + EPS)
    return (moment * scale).astype(jnp.bfloat16)

def reference(saved_input, query_cot, attn_out, out_cot, query_basis, output_basis, query_weight, output_weight, query_moment, output_moment):
    query_grad = jnp.dot(saved_input.T, query_cot, preferred_element_type=jnp.float32)
    query_proj = jnp.dot(query_basis.astype(jnp.float32).T, query_grad, precision=lax.Precision.HIGHEST)
    cot_proj = jnp.dot(out_cot, output_basis, preferred_element_type=jnp.float32)
    output_proj = jnp.dot(attn_out.astype(jnp.float32).T, cot_proj, precision=lax.Precision.HIGHEST)
    query_moment_new = BETA * query_moment + (1.0 - BETA) * query_proj
    output_moment_new = BETA * output_moment + (1.0 - BETA) * output_proj
    query_dir = normalize(query_moment_new)
    output_dir = normalize(output_moment_new)
    query_step = jnp.dot(query_basis, query_dir, preferred_element_type=jnp.float32)
    output_step = jnp.dot(output_dir, output_basis.T, preferred_element_type=jnp.float32)
    query_new = query_weight - RATE * query_step
    output_new = output_weight - RATE * output_step
    return (query_step, output_step, query_new, output_new, query_new.astype(jnp.bfloat16), output_new.astype(jnp.bfloat16), query_moment_new, output_moment_new)
```

```python
import jax
import jax.numpy as jnp
from jax import lax
from jax.experimental import pallas as pl
from jax.experimental.pallas import tpu as pltpu
from jax.sharding import PartitionSpec as P

BETA = 0.8
RATE = 0.2
EPS = 1e-06
BF16 = jnp.bfloat16
F32 = jnp.float32
SMEM = pl.BlockSpec(memory_space=pltpu.SMEM)
VMEM = pl.BlockSpec(memory_space=pltpu.VMEM)


def shift(x, axis, k):
    n = lax.axis_size(axis)
    return lax.ppermute(x, axis, [(i, (i + k) % n) for i in range(n)])


def flip(x, axis, m):
    return lax.ppermute(x, axis, [(i, i ^ m) for i in range(lax.axis_size(axis))])


def call(kernel, ids, args, outs, scratch=()):
    return pl.pallas_call(
        kernel,
        out_shape=outs,
        in_specs=[SMEM] + [VMEM] * len(args),
        out_specs=jax.tree.map(lambda _: VMEM, outs),
        scratch_shapes=scratch,
    )(ids, *args)


def project(ids, tokens, basis, own, mates):
    fs, reps = lax.axis_size("fs"), len(mates) + 1
    rows, half = basis.shape[0], own.shape[1]
    chunk = rows // reps

    def kernel(ids, tokens, basis, *rest):
        groups, out, whole = rest[:reps], rest[reps], rest[reps + 1]
        f, r, t = ids[0], ids[1], ids[2]
        whole[pl.ds(pl.multiple_of(f * rows, rows), rows), :] = basis[
            :, pl.ds(pl.multiple_of(t * half, half), half)
        ]
        for m, group in enumerate(groups):
            for k in range(1, fs):
                at = lax.rem(f + fs - k, fs) * rows + (r ^ m) * chunk
                whole[pl.ds(pl.multiple_of(at, chunk), chunk), :] = group[
                    (k - 1) * chunk : k * chunk, :
                ]
        out[...] = jnp.dot(tokens[...], whole[...], preferred_element_type=F32).astype(BF16)

    return call(
        kernel,
        ids,
        [tokens, basis, own, *mates],
        jax.ShapeDtypeStruct((tokens.shape[0], half), BF16),
        [pltpu.VMEM((fs * rows, half), BF16)],
    )


def contract(ids, mine, other, local, reps, flat):
    rows, half = mine.shape
    rank, width = 2 * half, local.shape[1]
    share = rank // reps
    shape = (width, share) if flat else (share, width)

    def kernel(ids, mine, other, local, keep, *rest):
        sends, both = rest[: reps - 1], rest[reps - 1]
        r, t = ids[1], ids[2]
        both[:, pl.ds(pl.multiple_of(t * half, half), half)] = mine[...]
        both[:, pl.ds(pl.multiple_of((1 - t) * half, half), half)] = other[...]
        for m in range(reps):
            part = both[:, pl.ds(pl.multiple_of((r ^ m) * share, share), share)]
            pair = (local[...], part) if flat else (part, local[...])
            block = lax.dot_general(*pair, (((0,), (0,)), ((), ())), preferred_element_type=F32)
            if m:
                sends[m - 1][...] = block.astype(BF16)
            else:
                keep[...] = block

    return call(
        kernel,
        ids,
        [mine, other, local],
        [jax.ShapeDtypeStruct(shape, F32)] + [jax.ShapeDtypeStruct(shape, BF16)] * (reps - 1),
        [pltpu.VMEM((rows, rank), BF16)],
    )


def add_and_split(ids, keep, terms):
    fs = lax.axis_size("fs")
    rows, width = keep.shape
    size = rows // fs

    def kernel(ids, keep, *rest):
        terms, own, sends, total = rest[: len(terms_)], rest[-fs - 1], rest[-fs:-1], rest[-1]
        f = ids[0]
        value = keep[...]
        for term in terms:
            value = value + term[...].astype(F32)
        total[...] = value
        for k in range(fs):
            at = pl.multiple_of(lax.rem(f + k, fs) * size, size)
            part = total[pl.ds(at, size), :]
            if k:
                sends[k - 1][...] = part.astype(BF16)
            else:
                own[...] = part

    terms_ = terms
    return call(
        kernel,
        ids,
        [keep, *terms],
        [jax.ShapeDtypeStruct((size, width), F32)]
        + [jax.ShapeDtypeStruct((size, width), BF16)] * (fs - 1),
        [pltpu.VMEM((rows, width), F32)],
    )


def advance(ids, moment, pieces):
    fs = len(pieces)
    rows, width = moment.shape
    size = rows // fs

    def kernel(ids, moment, *rest):
        pieces, (new, rounded, squares) = rest[:fs], rest[fs:]
        f = ids[0]
        for k, piece in enumerate(pieces):
            at = pl.ds(pl.multiple_of(lax.rem(f + fs - k, fs) * size, size), size)
            new[at, :] = BETA * moment[at, :] + (1.0 - BETA) * piece[...].astype(F32)
        value = new[...]
        rounded[...] = value.astype(BF16)
        value = jnp.sum((value * value).reshape(rows // 8, 8, width), axis=0)
        lanes = value[:, :128]
        for j in range(1, width // 128):
            lanes = lanes + value[:, j * 128 : (j + 1) * 128]
        squares[...] = lanes

    return call(
        kernel,
        ids,
        [moment, *pieces],
        [
            jax.ShapeDtypeStruct((rows, width), F32),
            jax.ShapeDtypeStruct((rows, width), BF16),
            jax.ShapeDtypeStruct((8, 128), F32),
        ],
    )


def finish(ids, squares, entries, basis, blocks, weight, flat):
    reps = len(blocks)
    rows, width = weight.shape
    rank = basis.shape[1]
    share = rank // reps
    tile = min(rows, 128)
    full = (rows, rank) if flat else (rank, width)

    def kernel(ids, squares, basis, *rest):
        blocks, weight, step, new, copy, whole = rest[:reps], *rest[reps:]
        r = ids[1]

        @pl.when(pl.program_id(0) == 0)
        def _():
            for m, block in enumerate(blocks):
                at = pl.ds(pl.multiple_of((r ^ m) * share, share), share)
                if flat:
                    whole[:, at] = block[...]
                else:
                    whole[at, :] = block[...]

        scale = lax.rsqrt(jnp.sum(squares[...]) * (1.0 / entries) + EPS)
        if flat:
            i = pl.multiple_of(pl.program_id(0) * tile, tile)
            value = lax.dot_general(
                whole[pl.ds(i, tile), :],
                basis[...],
                (((1,), (1,)), ((), ())),
                preferred_element_type=F32,
            )
        else:
            value = jnp.dot(basis[...], whole[...], preferred_element_type=F32)
        value = value * scale
        step[...] = value
        value = weight[...] - RATE * value
        new[...] = value
        copy[...] = value.astype(BF16)

    by_rows = pl.BlockSpec((tile, width), lambda i: (i, 0))
    basis_spec = VMEM if flat else pl.BlockSpec((tile, rank), lambda i: (i, 0))
    return pl.pallas_call(
        kernel,
        grid=(rows // tile,),
        out_shape=[
            jax.ShapeDtypeStruct(weight.shape, F32),
            jax.ShapeDtypeStruct(weight.shape, F32),
            jax.ShapeDtypeStruct(weight.shape, BF16),
        ],
        in_specs=[SMEM, VMEM, basis_spec] + [VMEM] * reps + [by_rows],
        out_specs=[by_rows] * 3,
        scratch_shapes=[pltpu.VMEM(full, BF16)],
    )(ids, squares, basis, *blocks, weight)


def stream(ids, tokens, local, basis, weight, moment, flat):
    fs, reps, tps = (lax.axis_size(axis) for axis in ("fs", "rep", "tp"))
    rows, rank = basis.shape
    chunk, half = rows // reps, rank // tps
    piece = lax.dynamic_slice(basis, (ids[1] * chunk, ids[2] * half), (chunk, half))
    own = jnp.concatenate([shift(piece, "fs", k) for k in range(1, fs)])
    mine = project(ids, tokens, basis, own, [flip(own, "rep", m) for m in range(1, reps)])
    keep, *sends = contract(ids, mine, flip(mine, "tp", 1), local, reps, flat)
    terms = [flip(send, "rep", m + 1) for m, send in enumerate(sends)]
    part, *sends = add_and_split(ids, keep, terms)
    for k, send in enumerate(sends):
        part = part + shift(send, "fs", k + 1).astype(F32)
    part = part.astype(BF16)
    new, rounded, squares = advance(
        ids, moment, [part] + [shift(part, "fs", k) for k in range(1, fs)]
    )
    blocks = [rounded] + [flip(rounded, "rep", m) for m in range(1, reps)]
    squares = squares + flip(squares, "tp", 1)
    bit = 1
    while bit < reps:
        squares = squares + flip(squares, "rep", bit)
        bit *= 2
    entries = moment.size * reps * tps
    return *finish(ids, squares, entries, basis, blocks, weight, flat), new


def direct(
    saved_input,
    query_cot,
    attn_out,
    out_cot,
    query_basis,
    output_basis,
    query_weight,
    output_weight,
    query_moment,
    output_moment,
):
    ids = jnp.stack([lax.axis_index(axis) for axis in ("fs", "rep", "tp")]).astype(jnp.int32)
    query_step, query_new, query_copy, query_moment_new = stream(
        ids, saved_input, query_cot, query_basis, query_weight, query_moment, False
    )
    output_step, output_new, output_copy, output_moment_new = stream(
        ids, out_cot, attn_out, output_basis, output_weight, output_moment, True
    )
    return (
        query_step,
        output_step,
        query_new,
        output_new,
        query_copy,
        output_copy,
        query_moment_new,
        output_moment_new,
    )


def on_device(
    saved_input,
    query_cot,
    attn_out,
    out_cot,
    query_basis,
    output_basis,
    query_weight,
    output_weight,
    query_moment,
    output_moment,
):
    rank = query_basis.shape[1]
    grad_rows = lax.psum_scatter(
        jnp.dot(saved_input.T, query_cot, preferred_element_type=jnp.float32),
        "fs",
        scatter_dimension=0,
        tiled=True,
    )
    query_part = jnp.dot(
        query_basis.astype(jnp.float32).T, grad_rows, precision=lax.Precision.HIGHEST
    )
    cot_proj = jnp.dot(
        out_cot,
        lax.all_gather(output_basis, "fs", axis=0, tiled=True),
        preferred_element_type=jnp.float32,
    )
    output_part = jnp.dot(attn_out.astype(jnp.float32).T, cot_proj, precision=lax.Precision.HIGHEST)
    reps = lax.axis_size("rep")
    share = rank // reps
    query_terms, output_terms = (
        lax.all_to_all(
            query_part.astype(jnp.bfloat16), "rep", split_axis=0, concat_axis=0, tiled=True
        ).astype(query_part.dtype),
        lax.all_to_all(
            output_part.T.astype(jnp.bfloat16), "rep", split_axis=0, concat_axis=0, tiled=True
        ).astype(jnp.float32),
    )
    width = query_part.shape[1]
    query_local = jnp.sum(query_terms.reshape(reps, share, width), axis=0)
    output_local = jnp.sum(output_terms.reshape(reps, share, width), axis=0)
    query_share, output_flip = lax.psum((query_local, output_local), "fs")
    output_share = output_flip.T
    query_moment_new = BETA * query_moment + (1.0 - BETA) * query_share
    output_moment_new = BETA * output_moment + (1.0 - BETA) * output_share
    query_squares, output_squares = lax.psum(
        (
            jnp.sum(query_moment_new * query_moment_new),
            jnp.sum(output_moment_new * output_moment_new),
        ),
        ("rep", "tp"),
    )
    entries = rank * query_moment.shape[1] * lax.axis_size("tp")
    query_dir = (query_moment_new * lax.rsqrt(query_squares / entries + EPS)).astype(jnp.bfloat16)
    output_dir = (output_moment_new * lax.rsqrt(output_squares / entries + EPS)).astype(
        jnp.bfloat16
    )
    query_full, output_full = (
        lax.all_gather(query_dir, "rep", axis=0, tiled=True),
        lax.all_gather(output_dir, "rep", axis=1, tiled=True),
    )
    query_step = jnp.dot(query_basis, query_full, preferred_element_type=jnp.float32)
    output_step = jnp.dot(output_full, output_basis.T, preferred_element_type=jnp.float32)
    query_new = query_weight - RATE * query_step
    output_new = output_weight - RATE * output_step
    return (
        query_step,
        output_step,
        query_new,
        output_new,
        query_new.astype(jnp.bfloat16),
        output_new.astype(jnp.bfloat16),
        query_moment_new,
        output_moment_new,
    )


def solution(mesh):
    placed = (
        P(("fs", "rep"), None),
        P(("fs", "rep"), "tp"),
        P(("fs", "rep"), "tp"),
        P(("fs", "rep"), None),
        P("fs", None),
        P("fs", None),
        P("fs", "tp"),
        P("tp", "fs"),
        P("rep", "tp"),
        P("tp", "rep"),
    )
    small = mesh.shape["fs"] <= 4 and mesh.shape["rep"] == 4 and mesh.shape["tp"] == 2
    return jax.shard_map(
        direct if small else on_device,
        mesh=mesh,
        in_specs=placed,
        out_specs=(
            P("fs", "tp"),
            P("tp", "fs"),
            P("fs", "tp"),
            P("tp", "fs"),
            P("fs", "tp"),
            P("tp", "fs"),
            P("rep", "tp"),
            P("tp", "rep"),
        ),
        check_vma=False,
    )
```

```python
import jax
import jax.numpy as jnp
from jax import lax
from jax.experimental import pallas as pl
from jax.experimental.pallas import tpu as pltpu
from jax.sharding import PartitionSpec as P

BETA = 0.8
RATE = 0.2
EPS = 1e-06
BF16 = jnp.bfloat16
F32 = jnp.float32
LIMIT = pltpu.CompilerParams(vmem_limit_bytes=16 * 2**20)
HBM = pl.BlockSpec(memory_space=pltpu.HBM)
GATHER = (0, 1, 2, 0)
SMEM = pl.BlockSpec(memory_space=pltpu.SMEM)
VMEM = pl.BlockSpec(memory_space=pltpu.VMEM)


def far(x):
    return pltpu.with_memory_space_constraint(x, pltpu.HBM)


def flip(x, axis, m):
    return lax.ppermute(x, axis, [(i, i ^ m) for i in range(lax.axis_size(axis))])


def call(kernel, ids, args, outs, scratch=()):
    return pl.pallas_call(
        kernel,
        out_shape=outs,
        in_specs=[SMEM] + [VMEM] * len(args),
        out_specs=jax.tree.map(lambda _: VMEM, outs),
        scratch_shapes=scratch,
        compiler_params=LIMIT,
    )(ids, *args)


def cut(ids, query_basis, output_basis, chunk, half):
    def kernel(ids, query_basis, output_basis, out, sems):
        at = (
            pl.ds(pl.multiple_of(ids[1] * chunk, chunk), chunk),
            pl.ds(pl.multiple_of(ids[2] * half, half), half),
        )
        copies = [
            pltpu.make_async_copy(basis.at[at], out.at[pl.ds(i * chunk, chunk), :], sems.at[i])
            for i, basis in enumerate((query_basis, output_basis))
        ]
        for copy in copies:
            copy.start()
        for copy in copies:
            copy.wait()

    return pl.pallas_call(
        kernel,
        out_shape=jax.ShapeDtypeStruct((2 * chunk, half), BF16),
        in_specs=[SMEM, HBM, HBM],
        out_specs=VMEM,
        scratch_shapes=[pltpu.SemaphoreType.DMA((2,))],
        compiler_params=LIMIT,
    )(ids, far(query_basis), far(output_basis))


def load(*arrays):
    def kernel(*refs):
        n = len(arrays)
        copies = [
            pltpu.make_async_copy(refs[i], refs[n + i], refs[2 * n].at[i]) for i in range(n)
        ]
        for copy in copies:
            copy.start()
        for copy in copies:
            copy.wait()

    return pl.pallas_call(
        kernel,
        out_shape=[jax.ShapeDtypeStruct(x.shape, x.dtype) for x in arrays],
        in_specs=[HBM] * len(arrays),
        out_specs=[VMEM] * len(arrays),
        scratch_shapes=[pltpu.SemaphoreType.DMA((len(arrays),))],
        compiler_params=LIMIT,
    )(*map(far, arrays))


def project(ids, tokens, bases, groups):
    fs, reps = len(groups) + 1, len(groups[0])
    rows = bases[0].shape[0]
    chunk, half = rows // reps, groups[0][0].shape[1]
    count = tokens[0].shape[0]
    flat = [piece for group in groups for piece in group]

    def kernel(ids, first, second, query_basis, output_basis, *rest):
        pieces, out = rest[: len(flat)], rest[len(flat)]
        f, r, t = ids[0], ids[1], ids[2]
        for i, (x, basis) in enumerate(((first, query_basis), (second, output_basis))):
            whole = rest[len(flat) + 1 + i]
            whole[pl.ds(pl.multiple_of(f * rows, rows), rows), :] = basis[
                :, pl.ds(pl.multiple_of(t * half, half), half)
            ]
            for k in range(1, fs):
                for m in range(reps):
                    at = (f ^ k) * rows + (r ^ m) * chunk
                    whole[pl.ds(pl.multiple_of(at, chunk), chunk), :] = pieces[
                        (k - 1) * reps + m
                    ][i * chunk : (i + 1) * chunk, :]
            out[i * count : (i + 1) * count, :] = jnp.dot(
                x[...], whole[...], preferred_element_type=F32
            ).astype(BF16)

    return call(
        kernel,
        ids,
        [*tokens, *bases, *flat],
        jax.ShapeDtypeStruct((2 * count, half), BF16),
        [pltpu.VMEM((fs * rows, half), BF16)] * 2,
    )


def contract(ids, mine, other, query_cot, attn_out, reps):
    count, half = mine.shape[0] // 2, mine.shape[1]
    rank, width = 2 * half, query_cot.shape[1]
    share = rank // reps
    tiles = width // share
    shape = (2 * width, share)

    def kernel(ids, mine, other, query_cot, attn_out, keep, *rest):
        sends, both = rest[: reps - 1], rest[reps - 1]
        r, t = ids[1], ids[2]
        both[:, pl.ds(pl.multiple_of(t * half, half), half)] = mine[...]
        both[:, pl.ds(pl.multiple_of((1 - t) * half, half), half)] = other[...]
        for m in (*range(1, reps), 0):
            out = sends[m - 1] if m else keep
            ranks = pl.ds(pl.multiple_of((r ^ m) * share, share), share)
            dims = (((0,), (0,)), ((), ()))
            block = lax.dot_general(
                both[:count, ranks], query_cot[...], dims, preferred_element_type=F32
            ).astype(out.dtype)
            for i in range(tiles):
                out[i * share : (i + 1) * share, :] = block[:, i * share : (i + 1) * share]
            out[width:, :] = lax.dot_general(
                attn_out[...], both[count:, ranks], dims, preferred_element_type=F32
            ).astype(out.dtype)

    return call(
        kernel,
        ids,
        [mine, other, query_cot, attn_out],
        [jax.ShapeDtypeStruct(shape, F32)] + [jax.ShapeDtypeStruct(shape, BF16)] * (reps - 1),
        [pltpu.VMEM((2 * count, rank), BF16)],
    )


def add_and_split(ids, keep, terms, fs):
    rows, width = keep.shape
    size = rows // (2 * fs)

    def kernel(ids, keep, *rest):
        terms, own, sends, total = rest[: -fs - 1], rest[-fs - 1], rest[-fs:-1], rest[-1]
        f = ids[0]
        value = keep[...]
        for term in terms:
            value = value + term[...].astype(F32)
        total[...] = value
        for k in (*range(1, fs), 0):
            at = pl.multiple_of((f ^ k) * size, size)
            out = sends[k - 1] if k else own
            for i in range(2):
                out[i * size : (i + 1) * size, :] = total[
                    pl.ds(at + i * rows // 2, size), :
                ].astype(out.dtype)

    return call(
        kernel,
        ids,
        [keep, *terms],
        [jax.ShapeDtypeStruct((2 * size, width), F32)]
        + [jax.ShapeDtypeStruct((2 * size, width), BF16)] * (fs - 1),
        [pltpu.VMEM((rows, width), F32)],
    )


def total(ids, own, terms):
    def kernel(ids, own, *rest):
        value = own[...]
        for term in rest[:-1]:
            value = value + term[...].astype(F32)
        rest[-1][...] = value.astype(BF16)

    return call(kernel, ids, [own, *terms], jax.ShapeDtypeStruct(own.shape, BF16))


def advance(ids, query_moment, output_moment, pieces):
    fs = len(pieces)
    size = output_moment.shape[0] // fs
    moments = (query_moment, output_moment)

    def kernel(ids, *rest):
        olds, pieces, news, (rounded, squares) = rest[:2], rest[2:-4], rest[-4:-2], rest[-2:]
        f = ids[0]
        for i in range(2):
            sums = jnp.zeros((8, pieces[0].shape[1]), F32)
            for k, piece in enumerate(pieces):
                start = pl.multiple_of((f ^ k) * size, size)
                ds = pl.ds(start, size)
                at = (slice(None), ds) if i == 0 else (ds, slice(None))
                value = BETA * olds[i][at] + (1.0 - BETA) * piece[
                    i * size : (i + 1) * size, :
                ].astype(F32)
                news[i][at] = value
                rounded[pl.ds(start + i * fs * size, size), :] = value.astype(BF16)
            value = news[i][...]
            value = jnp.sum((value * value).reshape(value.shape[0] // 8, 8, value.shape[1]), axis=0)
            for j in range(value.shape[1] // sums.shape[1]):
                sums = sums + value[:, j * sums.shape[1] : (j + 1) * sums.shape[1]]
            squares[8 * i : 8 * i + 8, :] = sums

    return call(
        kernel,
        ids,
        [*moments, *pieces],
        [jax.ShapeDtypeStruct(x.shape, F32) for x in moments]
        + [
            jax.ShapeDtypeStruct((2 * fs * size, pieces[0].shape[1]), BF16),
            jax.ShapeDtypeStruct((16, pieces[0].shape[1]), F32),
        ],
    )


def finish(ids, squares, entries, bases, blocks, weights):
    reps = len(blocks)
    rows, width = weights[0].shape
    rank = bases[0].shape[1]
    share = rank // reps
    tile = min(rows, 128)
    steps = rows // tile

    def kernel(ids, *rest):
        squares, query_basis, output_basis, *rest = rest
        blocks, rest = rest[:reps], rest[reps:]
        weights, outs, kept, (query_whole, output_whole, sems) = (
            rest[:2],
            rest[2:8],
            rest[8:14],
            rest[14:],
        )
        r = ids[1]
        for m in range(reps):
            at = pl.ds(pl.multiple_of((r ^ m) * share, share), share)
            for i in range(width // share):
                cols = slice(i * share, (i + 1) * share)
                query_whole[at, cols] = blocks[m][cols, :]
            output_whole[:, at] = blocks[m][width:, :]
        value = squares[...]
        copies = []
        for i in range(2):
            scale = lax.rsqrt(jnp.sum(value[8 * i : 8 * i + 8, :]) * (1.0 / entries) + EPS)
            for j in range(steps):
                at = slice(j * tile, (j + 1) * tile)
                if i == 0:
                    step = jnp.dot(
                        query_basis[at, :], query_whole[...], preferred_element_type=F32
                    )
                else:
                    step = lax.dot_general(
                        output_whole[at, :],
                        output_basis[...],
                        (((1,), (1,)), ((), ())),
                        preferred_element_type=F32,
                    )
                step = step * scale
                new = weights[i][at, :] - RATE * step
                for n, result in enumerate((step, new, new.astype(BF16))):
                    n = 3 * i + n
                    kept[n][at, :] = result
                    copies.append(
                        pltpu.make_async_copy(
                            kept[n].at[at, :], outs[n].at[at, :], sems.at[n * steps + j]
                        )
                    )
                    copies[-1].start()
        for copy in copies:
            copy.wait()

    kinds = (F32, F32, BF16) * 2
    args = [squares, *bases, *blocks, *weights]
    return pl.pallas_call(
        kernel,
        out_shape=[jax.ShapeDtypeStruct((rows, width), kind) for kind in kinds],
        in_specs=[SMEM] + [VMEM] * len(args),
        out_specs=[HBM] * 6,
        scratch_shapes=[pltpu.VMEM((rows, width), kind) for kind in kinds]
        + [
            pltpu.VMEM((rank, width), BF16),
            pltpu.VMEM((rows, rank), BF16),
            pltpu.SemaphoreType.DMA((6 * steps,)),
        ],
        compiler_params=LIMIT,
    )(ids, *args)


def gather(x, fewer):
    one, two = flip(x, "rep", 1), flip(x, "rep", 2)
    if fewer == 1:
        return [x, one, two, flip(one, "rep", 2)]
    if fewer == 2:
        return [x, one, two, flip(two, "rep", 1)]
    return [x, one, two, flip(x, "rep", 3)]


def direct(
    saved_input,
    query_cot,
    attn_out,
    out_cot,
    query_basis,
    output_basis,
    query_weight,
    output_weight,
    query_moment,
    output_moment,
):
    fs, reps, tps = (lax.axis_size(axis) for axis in ("fs", "rep", "tp"))
    ids = jnp.stack([lax.axis_index(axis) for axis in ("fs", "rep", "tp")]).astype(jnp.int32)
    rows, rank = query_basis.shape
    piece = cut(ids, query_basis, output_basis, rows // reps, rank // tps)
    groups = [gather(flip(piece, "fs", k), GATHER[k]) for k in range(1, fs)]
    tokens = load(saved_input, out_cot)
    mine = project(ids, tokens, (query_basis, output_basis), groups)
    keep, *sends = contract(ids, mine, flip(mine, "tp", 1), query_cot, attn_out, reps)
    terms = [flip(send, "rep", m + 1) for m, send in enumerate(sends)]
    own, *sends = add_and_split(ids, keep, terms, fs)
    part = total(ids, own, [flip(send, "fs", k + 1) for k, send in enumerate(sends)])
    pieces = [part] + [flip(part, "fs", k) for k in range(1, fs)]
    query_moment_new, output_moment_new, rounded, squares = advance(
        ids, query_moment, output_moment, pieces
    )
    blocks = gather(rounded, 0)
    squares = squares + flip(squares, "tp", 1)
    squares = squares + flip(squares, "rep", 1)
    squares = squares + flip(squares, "rep", 2)
    query_step, query_new, query_copy, output_step, output_new, output_copy = finish(
        ids,
        squares,
        query_moment.size * reps * tps,
        (query_basis, output_basis),
        blocks,
        (query_weight, output_weight),
    )
    return (
        query_step,
        output_step,
        query_new,
        output_new,
        query_copy,
        output_copy,
        query_moment_new,
        output_moment_new,
    )


def on_device(
    saved_input,
    query_cot,
    attn_out,
    out_cot,
    query_basis,
    output_basis,
    query_weight,
    output_weight,
    query_moment,
    output_moment,
):
    rank = query_basis.shape[1]
    grad_rows = lax.psum_scatter(
        jnp.dot(saved_input.T, query_cot, preferred_element_type=jnp.float32),
        "fs",
        scatter_dimension=0,
        tiled=True,
    )
    query_part = jnp.dot(
        query_basis.astype(jnp.float32).T, grad_rows, precision=lax.Precision.HIGHEST
    )
    cot_proj = jnp.dot(
        out_cot,
        lax.all_gather(output_basis, "fs", axis=0, tiled=True),
        preferred_element_type=jnp.float32,
    )
    output_part = jnp.dot(attn_out.astype(jnp.float32).T, cot_proj, precision=lax.Precision.HIGHEST)
    reps = lax.axis_size("rep")
    share = rank // reps
    query_terms, output_terms = (
        lax.all_to_all(
            query_part.astype(jnp.bfloat16), "rep", split_axis=0, concat_axis=0, tiled=True
        ).astype(query_part.dtype),
        lax.all_to_all(
            output_part.T.astype(jnp.bfloat16), "rep", split_axis=0, concat_axis=0, tiled=True
        ).astype(jnp.float32),
    )
    width = query_part.shape[1]
    query_local = jnp.sum(query_terms.reshape(reps, share, width), axis=0)
    output_local = jnp.sum(output_terms.reshape(reps, share, width), axis=0)
    query_share, output_flip = lax.psum((query_local, output_local), "fs")
    output_share = output_flip.T
    query_moment_new = BETA * query_moment + (1.0 - BETA) * query_share
    output_moment_new = BETA * output_moment + (1.0 - BETA) * output_share
    query_squares, output_squares = lax.psum(
        (
            jnp.sum(query_moment_new * query_moment_new),
            jnp.sum(output_moment_new * output_moment_new),
        ),
        ("rep", "tp"),
    )
    entries = rank * query_moment.shape[1] * lax.axis_size("tp")
    query_dir = (query_moment_new * lax.rsqrt(query_squares / entries + EPS)).astype(jnp.bfloat16)
    output_dir = (output_moment_new * lax.rsqrt(output_squares / entries + EPS)).astype(
        jnp.bfloat16
    )
    query_full, output_full = (
        lax.all_gather(query_dir, "rep", axis=0, tiled=True),
        lax.all_gather(output_dir, "rep", axis=1, tiled=True),
    )
    query_step = jnp.dot(query_basis, query_full, preferred_element_type=jnp.float32)
    output_step = jnp.dot(output_full, output_basis.T, preferred_element_type=jnp.float32)
    query_new = query_weight - RATE * query_step
    output_new = output_weight - RATE * output_step
    return (
        query_step,
        output_step,
        query_new,
        output_new,
        query_new.astype(jnp.bfloat16),
        output_new.astype(jnp.bfloat16),
        query_moment_new,
        output_moment_new,
    )


def solution(mesh):
    placed = (
        P(("fs", "rep"), None),
        P(("fs", "rep"), "tp"),
        P(("fs", "rep"), "tp"),
        P(("fs", "rep"), None),
        P("fs", None),
        P("fs", None),
        P("fs", "tp"),
        P("tp", "fs"),
        P("rep", "tp"),
        P("tp", "rep"),
    )
    small = mesh.shape["fs"] == 4 and mesh.shape["rep"] == 4 and mesh.shape["tp"] == 2
    return jax.shard_map(
        direct if small else on_device,
        mesh=mesh,
        in_specs=placed,
        out_specs=(
            P("fs", "tp"),
            P("tp", "fs"),
            P("fs", "tp"),
            P("tp", "fs"),
            P("fs", "tp"),
            P("tp", "fs"),
            P("rep", "tp"),
            P("tp", "rep"),
        ),
        check_vma=False,
    )
```
